32 devices in a mesh: ep: 4 (over y, x), tp: 8 (over z, core).
Axes of the slice: x: 2, y: 2, z: 4, core: 2. Of those that a mesh axis runs over, the one named last changes fastest.
Arguments:
- mixer_input: bfloat16 [6144, 1024], P(('ep', 'tp')), may hold values from -6 to 6
- mixer_gain: float32 [1024], replicated, may hold values from 0.1 to 1.9
- group_weight: bfloat16 [4, 256, 256], replicated, may hold values from -0.375 to 0.375
- mixer_scale: float32 [1024], replicated, may hold values from 0.1 to 1.9
- expert_input: bfloat16 [6144, 1024], P(('ep', 'tp')), may hold values from -6 to 6
- expert_gain: float32 [1024], replicated, may hold values from 0.1 to 1.9
- routes: int32 [6144, 2], P(('ep', 'tp')), may hold values from 0 to 3, all different within a row; in each aligned block of 192 rows (0 to 191, 192 to 383, ...) at most 144 rows name the same one
- route_weight: float32 [6144, 2], P(('ep', 'tp')), may hold values from 0.2 to 1
- w_gate: bfloat16 [4, 1024, 4096], P('ep', None, 'tp'), may hold values from -0.1875 to 0.1875
- w_up: bfloat16 [4, 1024, 4096], P('ep', None, 'tp'), may hold values from -0.1875 to 0.1875
- w_down: bfloat16 [4, 4096, 1024], P('ep', 'tp'), may hold values from -0.09375 to 0.09375
Outputs:
- mixer_out: bfloat16 [6144, 1024], P(('ep', 'tp'))
- expert_out: bfloat16 [6144, 1024], P(('ep', 'tp'))
The draws below stay inside these ranges and needn't reach their ends.
Inputs may be any that keep to these rules, and one draw needn't show every extreme that they name: `routes`: each row names 2 different experts. Among the rows of one device no expert is named by more than 144 rows, and in some device's rows some expert is named exactly 144 times.
All inputs are finite; a program needn't handle non-finite values.
Results may differ from the reference program's by a relative error of at most 0.0076.
Values may be sent and summed in bfloat16 or wider, within the bound.
No kernel may reach another device: no remote copies, remote signals or barrier semaphores. Data moves between devices by JAX's collectives and lax.ppermute only.
A program may use at most 128 MiB of HBM per device.

```python
import math
import jax
import jax.numpy as jnp
import numpy as np
from jax import lax

D = 1024
GROUP_WIDTH = 256
FFE = 4096
TOPK = 2
TOK_DEV = 192
EXPERTS = 4
CAP = 144
TOKENS = 6144
N_TP = 8
DEVICES = 32


def block_levels(rng, dims, pieces, low, largest):
    factor_of = 1.0
    for dim, blocks in pieces:
        heights = jax.random.uniform(jax.random.fold_in(jax.random.fold_in(rng, 6), dim), (blocks,), jnp.float32, low / len(pieces), largest / len(pieces))
        factor_of = factor_of * jnp.repeat(jnp.exp(heights), dims[dim] // blocks).reshape((-1,) + (1,) * (len(dims) - 1 - dim))
    return factor_of


def deal_out(own_key, own, number, rows, amount, top, bound, lean):
    ranking = jax.random.permutation(own_key, amount)
    crowded, ordinary = shares(amount, rows * top, bound, lean, True), shares(amount, rows * top, bound, lean, False)
    places = jnp.arange(amount)

    def named(tallies, turn):
        used = int((tallies > 0).sum())
        fixed = max(1, used // 4)
        passed = fixed + (places - fixed + turn * (used - fixed)) % max(1, amount - fixed)
        return jnp.zeros((amount,), jnp.int32).at[ranking[jnp.where(places < fixed, places, passed)]].set(jnp.asarray(tallies, jnp.int32))

    tallies = jnp.where(number % 4 == 0, named(crowded, number // 4), named(ordinary, number - number // 4 - 1))
    mixed = jax.random.permutation(jax.random.fold_in(own, 3), amount)
    giver, taker = mixed[0:amount // 2 * 2:2], mixed[1:amount // 2 * 2:2]
    room = jnp.minimum(tallies[giver] - 1, bound - tallies[taker]) // 2
    room = jnp.where((giver == ranking[0]) | (taker == ranking[0]) | (tallies[taker] == 0), 0, jnp.maximum(room, 0))
    passed = jax.random.randint(jax.random.fold_in(own, 4), (amount // 2,), 0, 1 << 20) % (room + 1)
    tallies = tallies.at[giver].add(-passed).at[taker].add(passed)
    labels = jnp.searchsorted(jnp.cumsum(tallies), jnp.arange(rows * top), side="right").astype(jnp.int32)
    listing = labels.reshape(top, rows).T
    listing = listing[jax.random.permutation(jax.random.fold_in(own, 1), rows)]
    turn = jax.random.randint(jax.random.fold_in(own, 2), (rows, 1), 0, top)
    return jnp.take_along_axis(listing, (jnp.arange(top)[None, :] + turn) % top, axis=1)


def shares(count, total, most, lean, full):
    portions = [(1 << 20) // math.isqrt(rank ** lean) + 1 for rank in range(1, count + 1)]
    largest = most if full else min(most, max(-(-total // count), total * portions[0] // sum(portions)))
    least = 1 if total - largest >= count - 1 else 0
    given, spare = [largest] + [least] * (count - 1), total - largest - least * (count - 1)
    while spare > 0:
        free = [i for i in range(1, count) if given[i] < largest] or [i for i in range(1, count) if given[i] < most]
        pool, budget = sum([portions[i] for i in free]), spare
        for i in free:
            more = min(most - given[i], max(1, budget * portions[i] // pool), spare)
            given[i] = given[i] + more
            spare = spare - more
    return np.array(given)


def normal_values(stream_key, dims, width, bound, shards=(), kind=jnp.bfloat16):
    values = jax.random.normal(stream_key, dims, jnp.float32) * width
    if len(shards) > 0:
        values = block_levels(stream_key, dims, shards, -0.22, 0.18) * values
    return jnp.clip(values, min=-bound, max=bound).astype(kind)


def setup_inputs(seed: int = 0) -> dict:
    key_of = jax.random.split(jax.random.key(seed), 12)
    mixer_input = normal_values(key_of[0], (TOKENS, D), 1.0, 6.0, ((0, 32),))
    mixer_gain = jnp.clip(1.0 + 0.18 * jax.random.normal(key_of[1], (D,), jnp.float32), 0.1, 1.9)
    group_weight = normal_values(key_of[2], (4, GROUP_WIDTH, GROUP_WIDTH), GROUP_WIDTH ** -0.5, 0.375)
    mixer_scale = jnp.clip(1.0 + 0.18 * jax.random.normal(key_of[3], (D,), jnp.float32), 0.1, 1.9)
    expert_input = normal_values(key_of[4], (TOKENS, D), 1.0, 6.0, ((0, 32),))
    expert_gain = jnp.clip(1.0 + 0.18 * jax.random.normal(key_of[5], (D,), jnp.float32), 0.1, 1.9)
    routes_keys = jax.random.split(jax.random.fold_in(key_of[6], 1), TOKENS // TOK_DEV)
    routes_turns = jax.random.permutation(jax.random.fold_in(key_of[6], 3), TOKENS // TOK_DEV)
    routes = jax.vmap(lambda own, number: deal_out(jax.random.fold_in(key_of[6], 2), own, number, TOK_DEV, EXPERTS, TOPK, CAP, 2))(routes_keys, routes_turns).reshape((TOKENS, TOPK))
    route_weight = jnp.clip(0.2 + 0.8 * jax.random.uniform(key_of[7], (TOKENS, TOPK), jnp.float32) ** block_levels(key_of[7], (TOKENS, TOPK), ((0, 32),), -0.2, 0.2), 0.2, 1.0)
    w_gate = normal_values(key_of[8], (EXPERTS, D, FFE), D ** -0.5, 0.1875, ((0, 4), (2, 8)))
    w_up = normal_values(key_of[9], (EXPERTS, D, FFE), D ** -0.5, 0.1875, ((0, 4), (2, 8)))
    w_down = normal_values(key_of[10], (EXPERTS, FFE, D), FFE ** -0.5, 0.09375, ((0, 4), (1, 8)))
    return dict(mixer_input=mixer_input, mixer_gain=mixer_gain, group_weight=group_weight, mixer_scale=mixer_scale, expert_input=expert_input, expert_gain=expert_gain, routes=routes, route_weight=route_weight, w_gate=w_gate, w_up=w_up, w_down=w_down)


epsilon = 1e-06

def normalize(row_values, gain):
    values = row_values.astype(jnp.float32)
    scaled = values * lax.rsqrt(lax.optimization_barrier(jnp.mean(values * values, axis=-1, keepdims=True)) + epsilon)
    return (scaled * gain).astype(jnp.bfloat16)

def pool_groups(padded, start_row, row_count, seq_length):
    group_width = padded.shape[1] // 4
    position = start_row + jnp.arange(row_count, dtype=jnp.int32)
    centre = padded[8:8 + row_count]
    pooled_parts = []
    for group_index in range(4):
        window = 2 ** (group_index + 1)
        reach_left = window // 2
        reach_right = window - 1 - reach_left
        group_cols = padded[:, group_index * group_width:(group_index + 1) * group_width]
        window_sum = group_cols[8 - reach_left:8 - reach_left + row_count]
        for offset in range(1 - reach_left, reach_right + 1):
            window_sum = window_sum + group_cols[8 + offset:8 + offset + row_count]
        cover = (jnp.minimum(position + reach_right + 1, seq_length) - jnp.maximum(position - reach_left, 0)).astype(jnp.float32)
        pooled_parts.append(window_sum / cover[:, None] - centre[:, group_index * group_width:(group_index + 1) * group_width])
    return jnp.stack(pooled_parts, axis=1).astype(jnp.bfloat16)

def reference(mixer_input, mixer_gain, group_weight, mixer_scale, expert_input, expert_gain, routes, route_weight, w_gate, w_up, w_down):
    normed = normalize(mixer_input, mixer_gain)
    padded = jnp.pad(normed.astype(jnp.float32), ((8, 8), (0, 0)))
    pooled = pool_groups(padded, 0, TOKENS, TOKENS)
    mixed_groups = jnp.einsum('tgi,gio->tgo', pooled.astype(jnp.float32), group_weight.astype(jnp.float32))
    mixer_out = (mixed_groups.reshape(TOKENS, D) * mixer_scale).astype(jnp.bfloat16)
    expert_normed = normalize(expert_input, expert_gain)
    flat_route = routes.reshape(-1).astype(jnp.int32)
    flat_weight = route_weight.reshape(-1)
    most_rows = DEVICES * CAP
    block_width = FFE // N_TP

    def one_expert(running_out, inputs):
        gate_w, up_w, down_w, expert_index = inputs
        matches = flat_route == expert_index
        chosen = jnp.nonzero(matches, size=most_rows, fill_value=0)[0].astype(jnp.int32)
        live_rows = (jnp.arange(most_rows, dtype=jnp.int32) < jnp.sum(matches.astype(jnp.int32))).astype(jnp.float32)
        token_index = chosen // TOPK
        row_values = jnp.take(expert_normed, token_index, axis=0)
        gate_part = jnp.dot(row_values, gate_w, preferred_element_type=jnp.float32)
        up_part = jnp.dot(row_values, up_w, preferred_element_type=jnp.float32)
        hidden = (jax.nn.silu(gate_part) * up_part).astype(jnp.bfloat16)
        hidden_blocks = jnp.transpose(hidden.reshape(most_rows, N_TP, block_width), (1, 0, 2))
        weight_blocks = down_w.reshape(N_TP, block_width, D)

        def add_block(running, block_pair):
            hidden_block, weight_block = block_pair
            block_partial = lax.optimization_barrier(jnp.dot(hidden_block, weight_block, preferred_element_type=jnp.float32).astype(jnp.bfloat16))
            return (running + block_partial.astype(jnp.float32), None)
        summed, _ = lax.scan(add_block, jnp.zeros((most_rows, D), jnp.float32), (hidden_blocks, weight_blocks))
        expert_result = lax.optimization_barrier(summed.astype(jnp.bfloat16)).astype(jnp.float32)
        weights_here = jnp.take(flat_weight, chosen) * live_rows
        return (running_out.at[token_index].add(weights_here[:, None] * expert_result), None)
    total_out, _ = lax.scan(one_expert, jnp.zeros((TOKENS, D), jnp.float32), (w_gate, w_up, w_down, jnp.arange(EXPERTS, dtype=jnp.int32)))
    return (mixer_out, total_out.astype(jnp.bfloat16))
```

```python
import jax
import jax.numpy as jnp
from jax import lax
from jax.sharding import PartitionSpec as P

epsilon = 1e-06


def padded_2(value, sides, width):
    for axis, dim in sides:
        size, length = (lax.axis_size(axis), value.shape[dim])
        up = [(i, (i + 1) % size) for i in range(size - 1)]
        down = [(j, i) for i, j in up]
        last = lax.slice_in_dim(value, length - width, length, axis=dim)
        leading = lax.slice_in_dim(value, 0, width, axis=dim)
        before = lax.ppermute(last, axis, up)
        after = lax.ppermute(leading, axis, down)
        value = jnp.concatenate([before, value, after], axis=dim)
    return value


def normalize(row_values, gain):
    values = row_values.astype(jnp.float32)
    scaled = values * lax.rsqrt(jnp.mean(values * values, axis=-1, keepdims=True) + epsilon)
    return (scaled * gain).astype(jnp.bfloat16)


def pool_groups(padded, start_row, row_count, seq_length):
    group_width = padded.shape[1] // 4
    position = start_row + jnp.arange(row_count, dtype=jnp.int32)
    centre = padded[8 : 8 + row_count]
    pooled_parts = []
    for group_index in range(4):
        window = 2 ** (group_index + 1)
        reach_left = window // 2
        reach_right = window - 1 - reach_left
        group_cols = padded[:, group_index * group_width : (group_index + 1) * group_width]
        window_sum = group_cols[8 - reach_left : 8 - reach_left + row_count]
        for offset in range(1 - reach_left, reach_right + 1):
            window_sum = window_sum + group_cols[8 + offset : 8 + offset + row_count]
        cover = (
            jnp.minimum(position + reach_right + 1, seq_length)
            - jnp.maximum(position - reach_left, 0)
        ).astype(jnp.float32)
        pooled_parts.append(
            window_sum / cover[:, None]
            - centre[:, group_index * group_width : (group_index + 1) * group_width]
        )
    return jnp.stack(pooled_parts, axis=1).astype(jnp.bfloat16)


def mixer(mixer_input, mixer_gain, group_weight, mixer_scale):
    row_count = mixer_input.shape[0]
    normed = normalize(mixer_input, mixer_gain)
    padded = padded_2(normed, ((("ep", "tp"), 0),), 8)
    start_row = lax.axis_index(("ep", "tp")) * row_count
    seq_length = row_count * lax.axis_size(("ep", "tp"))
    pooled = pool_groups(padded.astype(jnp.float32), start_row, row_count, seq_length)
    mixed_groups = jnp.einsum(
        "tgi,gio->tgo", pooled, group_weight, preferred_element_type=jnp.float32
    )
    return (mixed_groups.reshape(row_count, -1) * mixer_scale).astype(jnp.bfloat16)


def swap(value, stride):
    size = lax.axis_size("tp")
    return lax.ppermute(value, "tp", [(i, i ^ stride) for i in range(size)])


def route_table(routes, route_weight, experts, capacity):
    row_count, top_count = routes.shape
    named = routes.T
    member = jnp.zeros((experts, row_count), jnp.float32)
    expert_ids = jnp.arange(experts, dtype=jnp.int32)[:, None]
    for k in range(top_count):
        member = member + (named[k][None, :] == expert_ids)
    earlier = (
        jnp.arange(row_count, dtype=jnp.int32)[:, None]
        < jnp.arange(row_count, dtype=jnp.int32)[None, :]
    )
    place = jnp.dot(
        member.astype(jnp.bfloat16),
        earlier.astype(jnp.bfloat16),
        preferred_element_type=jnp.float32,
    )
    place = place + expert_ids.astype(jnp.float32) * capacity
    slots = [
        jnp.sum(jnp.where(named[k][None, :] == expert_ids, place, 0.0), axis=0)
        for k in range(top_count)
    ]
    return jnp.concatenate([jnp.stack(slots), route_weight.T], axis=0)


def slot_hits(table, top_count, slots):
    ids = lax.broadcasted_iota(jnp.int32, (slots, table.shape[1]), 0).astype(jnp.float32)
    return [table[k][None, :] == ids for k in range(top_count)]


def dispatch(rows, table, top_count, slots):
    hits = slot_hits(table, top_count, slots)
    chosen = hits[0]
    for hit in hits[1:]:
        chosen = chosen | hit
    return jnp.dot(
        chosen.astype(jnp.bfloat16), rows, preferred_element_type=jnp.float32
    ).astype(jnp.bfloat16)


def combine(returned, table, top_count):
    hits = slot_hits(table, top_count, returned.shape[0])
    weight = jnp.zeros(hits[0].shape, jnp.float32)
    for k in range(top_count):
        weight = weight + jnp.where(hits[k], table[top_count + k][None, :], 0.0)
    high = lax.reduce_precision(weight, 8, 7)
    low = weight - high
    dims = (((0,), (0,)), ((), ()))
    parts = [
        lax.dot_general(
            part.astype(jnp.bfloat16), returned, dims, preferred_element_type=jnp.float32
        )
        for part in (high, low)
    ]
    return parts[0] + parts[1]


def over_experts(value):
    return lax.all_to_all(value, "ep", split_axis=0, concat_axis=0, tiled=True)


def on_device(
    mixer_input,
    mixer_gain,
    group_weight,
    mixer_scale,
    expert_input,
    expert_gain,
    routes,
    route_weight,
    w_gate,
    w_up,
    w_down,
):
    row_count, top_count = routes.shape
    experts = lax.axis_size("ep") * w_gate.shape[0]
    capacity = 3 * top_count * row_count // (2 * experts)
    slots = experts * capacity
    half = lax.axis_size("tp") // 2

    normed = normalize(expert_input, expert_gain)
    far_rows = swap(normed, half)

    shards = [(w_gate[0], w_up[0], w_down[0])]
    stride = half // 2
    while stride:
        shards = shards + [tuple(swap(w, stride) for w in shard) for shard in shards]
        stride //= 2

    table = route_table(routes, route_weight, experts, capacity)
    far_table = swap(table, half)
    near = over_experts(dispatch(normed, table, top_count, slots))
    far = over_experts(dispatch(far_rows, far_table, top_count, slots))

    def ffn(arrived):
        total = None
        for gate, up, down in shards:
            gate_part = jnp.dot(arrived, gate, preferred_element_type=jnp.float32)
            up_part = jnp.dot(arrived, up, preferred_element_type=jnp.float32)
            hidden = (jax.nn.silu(gate_part) * up_part).astype(jnp.bfloat16)
            term = jnp.dot(hidden, down, preferred_element_type=jnp.float32)
            total = term if total is None else total + term
        return total.astype(jnp.bfloat16)

    far_back = over_experts(ffn(far))
    far_sum = combine(far_back, far_table, top_count).astype(jnp.bfloat16)
    far_sum = swap(far_sum, half)
    near_back = over_experts(ffn(near))
    near_sum = combine(near_back, table, top_count)
    expert_out = (near_sum + far_sum.astype(jnp.float32)).astype(jnp.bfloat16)

    mixer_out = mixer(mixer_input, mixer_gain, group_weight, mixer_scale)
    return (mixer_out, expert_out)


def solution(mesh):
    placed = (
        P(("ep", "tp"), None),
        P(),
        P(),
        P(),
        P(("ep", "tp"), None),
        P(),
        P(("ep", "tp"), None),
        P(("ep", "tp"), None),
        P("ep", None, "tp"),
        P("ep", None, "tp"),
        P("ep", "tp", None),
    )

    return jax.shard_map(
        on_device,
        mesh=mesh,
        in_specs=placed,
        out_specs=(P(("ep", "tp"), None), P(("ep", "tp"), None)),
        check_vma=False,
    )
```

```python
import jax
import jax.numpy as jnp
from jax import lax
from jax.experimental import pallas as pl
from jax.experimental.pallas import tpu as pltpu
from jax.sharding import PartitionSpec as P

epsilon = 1e-06


def padded_2(value, sides, width):
    for axis, dim in sides:
        size, length = (lax.axis_size(axis), value.shape[dim])
        up = [(i, (i + 1) % size) for i in range(size - 1)]
        down = [(j, i) for i, j in up]
        last = lax.slice_in_dim(value, length - width, length, axis=dim)
        leading = lax.slice_in_dim(value, 0, width, axis=dim)
        before = lax.ppermute(last, axis, up)
        after = lax.ppermute(leading, axis, down)
        value = jnp.concatenate([before, value, after], axis=dim)
    return value


def normalize(row_values, gain):
    values = row_values.astype(jnp.float32)
    scaled = values * lax.rsqrt(jnp.mean(values * values, axis=-1, keepdims=True) + epsilon)
    return (scaled * gain).astype(jnp.bfloat16)


def pool_groups(padded, start_row, row_count, seq_length):
    group_width = padded.shape[1] // 4
    position = start_row + jnp.arange(row_count, dtype=jnp.int32)
    centre = padded[8 : 8 + row_count]
    pooled_parts = []
    for group_index in range(4):
        window = 2 ** (group_index + 1)
        reach_left = window // 2
        reach_right = window - 1 - reach_left
        group_cols = padded[:, group_index * group_width : (group_index + 1) * group_width]
        window_sum = group_cols[8 - reach_left : 8 - reach_left + row_count]
        for offset in range(1 - reach_left, reach_right + 1):
            window_sum = window_sum + group_cols[8 + offset : 8 + offset + row_count]
        cover = (
            jnp.minimum(position + reach_right + 1, seq_length)
            - jnp.maximum(position - reach_left, 0)
        ).astype(jnp.float32)
        pooled_parts.append(
            window_sum / cover[:, None]
            - centre[:, group_index * group_width : (group_index + 1) * group_width]
        )
    return jnp.stack(pooled_parts, axis=1).astype(jnp.bfloat16)


def mixer(mixer_input, mixer_gain, group_weight, mixer_scale):
    row_count = mixer_input.shape[0]
    normed = normalize(mixer_input, mixer_gain)
    padded = padded_2(normed, ((("ep", "tp"), 0),), 8)
    start_row = lax.axis_index(("ep", "tp")) * row_count
    seq_length = row_count * lax.axis_size(("ep", "tp"))
    pooled = pool_groups(padded.astype(jnp.float32), start_row, row_count, seq_length)
    mixed_groups = jnp.einsum(
        "tgi,gio->tgo", pooled, group_weight, preferred_element_type=jnp.float32
    )
    return (mixed_groups.reshape(row_count, -1) * mixer_scale).astype(jnp.bfloat16)


CORES = 2


def ring(value):
    size = lax.axis_size("tp")
    return lax.ppermute(value, "tp", [(i, (i + CORES) % size) for i in range(size)])


def core_swap(value):
    size = lax.axis_size("tp")
    return lax.ppermute(value, "tp", [(i, i ^ 1) for i in range(size)])


def is_direct(experts):
    return experts <= 4


def exchange(pieces):
    count = len(pieces)
    if is_direct(count):
        received = {
            m: lax.ppermute(pieces[m], "ep", [(i, i ^ m) for i in range(count)])
            for m in reversed(range(1, count))
        }
        return [pieces[0]] + [received[m] for m in range(1, count)]
    joined = lax.all_to_all(
        jnp.stack(pieces), "ep", split_axis=0, concat_axis=0, tiled=True
    )
    return [joined[m] for m in range(count)]


def route_table(routes, route_weight, experts, capacity):
    row_count, top_count = routes.shape
    named = routes.T
    if is_direct(experts):
        named = named ^ lax.axis_index("ep")
    member = jnp.zeros((experts, row_count), jnp.float32)
    expert_ids = jnp.arange(experts, dtype=jnp.int32)[:, None]
    for k in range(top_count):
        member = member + (named[k][None, :] == expert_ids)
    earlier = (
        jnp.arange(row_count, dtype=jnp.int32)[:, None]
        < jnp.arange(row_count, dtype=jnp.int32)[None, :]
    )
    place = jnp.dot(
        member.astype(jnp.bfloat16),
        earlier.astype(jnp.bfloat16),
        preferred_element_type=jnp.float32,
    )
    place = place + expert_ids.astype(jnp.float32) * capacity
    slots = [
        jnp.sum(jnp.where(named[k][None, :] == expert_ids, place, 0.0), axis=0)
        for k in range(top_count)
    ]
    return jnp.concatenate([jnp.stack(slots), route_weight.T], axis=0)


def slot_hits(table_ref, top_count, first, capacity):
    row_count = table_ref.shape[1]
    ids = lax.broadcasted_iota(jnp.int32, (capacity, row_count), 0) + first
    ids = ids.astype(jnp.float32)
    return [table_ref[k : k + 1, :] == ids for k in range(top_count)]


def dispatch(rows, table, experts, capacity):
    top_count = table.shape[0] // 2

    def kernel(rows_ref, table_ref, *out_refs):
        for m, out_ref in enumerate(out_refs):
            hits = slot_hits(table_ref, top_count, m * capacity, capacity)
            chosen = jnp.zeros(hits[0].shape, jnp.float32)
            for hit in hits:
                chosen = chosen + jnp.where(hit, 1.0, 0.0)
            out_ref[...] = jnp.dot(
                chosen.astype(jnp.bfloat16),
                rows_ref[...],
                preferred_element_type=jnp.float32,
            ).astype(jnp.bfloat16)

    shape = jax.ShapeDtypeStruct((capacity, rows.shape[1]), jnp.bfloat16)
    work = experts * capacity * rows.shape[0] * rows.shape[1]
    return pl.pallas_call(
        kernel,
        out_shape=[shape] * experts,
        cost_estimate=pl.CostEstimate(
            flops=2 * work, transcendentals=0, bytes_accessed=2 * rows.size + 2 * experts * shape.size
        ),
        name="dispatch",
    )(rows, table)


def combine(pieces, table, incoming):
    top_count = table.shape[0] // 2
    capacity, width = pieces[0].shape
    row_count = table.shape[1]
    extra = [] if incoming is None else [incoming]

    def kernel(table_ref, *refs):
        out_ref = refs[-1]
        total = jnp.zeros((row_count, width), jnp.float32)
        if extra:
            total = refs[-2][...].astype(jnp.float32)
        for m in range(len(pieces)):
            hits = slot_hits(table_ref, top_count, m * capacity, capacity)
            weight = jnp.zeros(hits[0].shape, jnp.float32)
            for k, hit in enumerate(hits):
                weight = weight + jnp.where(hit, table_ref[top_count + k : top_count + k + 1, :], 0.0)
            high = weight.astype(jnp.bfloat16)
            low = (weight - high.astype(jnp.float32)).astype(jnp.bfloat16)
            for part in (high, low):
                total = total + lax.dot_general(
                    part,
                    refs[m][...],
                    (((0,), (0,)), ((), ())),
                    preferred_element_type=jnp.float32,
                )
        out_ref[...] = total.astype(jnp.bfloat16)

    work = len(pieces) * capacity * row_count * width
    return pl.pallas_call(
        kernel,
        out_shape=jax.ShapeDtypeStruct((row_count, width), jnp.bfloat16),
        cost_estimate=pl.CostEstimate(
            flops=4 * work, transcendentals=0, bytes_accessed=2 * (len(pieces) * capacity + 2 * row_count) * width
        ),
        name="combine",
    )(table, *pieces, *extra)


def ffn(pieces, shards):
    count = len(pieces)
    capacity, width = pieces[0].shape
    rows = count * capacity
    hidden_width = shards[0][0].shape[1]
    tile = min(256, hidden_width)
    steps = hidden_width // tile
    n_shards = len(shards)

    def kernel(*refs):
        piece_refs = refs[:count]
        weight_refs = refs[count : count + 3 * n_shards]
        out_refs = refs[count + 3 * n_shards : 2 * count + 3 * n_shards]
        rows_ref, sum_ref = refs[-2:]
        step = pl.program_id(0)

        @pl.when(step == 0)
        def _():
            for m in range(count):
                rows_ref[m * capacity : (m + 1) * capacity, :] = piece_refs[m][...]

        values = rows_ref[...]
        term = None
        for n in range(n_shards):
            gate_ref, up_ref, down_ref = weight_refs[3 * n : 3 * n + 3]
            gate = jnp.dot(values, gate_ref[...], preferred_element_type=jnp.float32)
            up = jnp.dot(values, up_ref[...], preferred_element_type=jnp.float32)
            hidden = (gate / (1.0 + jnp.exp(-gate)) * up).astype(jnp.bfloat16)
            part = jnp.dot(hidden, down_ref[...], preferred_element_type=jnp.float32)
            term = part if term is None else term + part

        @pl.when(step == 0)
        def _():
            sum_ref[...] = term

        @pl.when(step > 0)
        def _():
            sum_ref[...] += term

        @pl.when(step == steps - 1)
        def _():
            for m in range(count):
                out_refs[m][...] = sum_ref[m * capacity : (m + 1) * capacity, :].astype(jnp.bfloat16)

    whole = pl.BlockSpec((capacity, width), lambda j: (0, 0))
    across = pl.BlockSpec((width, tile), lambda j: (0, j))
    along = pl.BlockSpec((tile, width), lambda j: (j, 0))
    work = rows * width * hidden_width * n_shards
    return pl.pallas_call(
        kernel,
        grid=(steps,),
        in_specs=[whole] * count + [across, across, along] * n_shards,
        out_specs=[whole] * count,
        out_shape=[jax.ShapeDtypeStruct((capacity, width), jnp.bfloat16)] * count,
        scratch_shapes=[
            pltpu.VMEM((rows, width), jnp.bfloat16),
            pltpu.VMEM((rows, width), jnp.float32),
        ],
        cost_estimate=pl.CostEstimate(
            flops=6 * work, transcendentals=rows * hidden_width * n_shards,
            bytes_accessed=4 * rows * width + 6 * width * hidden_width * n_shards,
        ),
        name="ffn",
    )(*pieces, *(w for shard in shards for w in shard))


def on_device(
    mixer_input,
    mixer_gain,
    group_weight,
    mixer_scale,
    expert_input,
    expert_gain,
    routes,
    route_weight,
    w_gate,
    w_up,
    w_down,
):
    row_count, top_count = routes.shape
    experts = lax.axis_size("ep") * w_gate.shape[0]
    capacity = 3 * top_count * row_count // (2 * experts)
    capacity = -(-capacity // 16) * 16
    chips = lax.axis_size("tp") // CORES

    normed = normalize(expert_input, expert_gain)
    shard = (w_gate[0], w_up[0], w_down[0])
    shards = [shard, tuple(core_swap(w) for w in shard)]

    table = route_table(routes, route_weight, experts, capacity)
    blocks, tables = [normed], [table]
    for _ in range(1, chips):
        blocks.append(ring(blocks[-1]))
        tables.append(ring(tables[-1]))

    back = []
    for n in range(chips):
        arrived = exchange(dispatch(blocks[n], tables[n], experts, capacity))
        served = ffn(arrived, shards)
        back.append(exchange(served))

    total = None
    for n in list(range(1, chips)) + [0]:
        total = combine(back[n], tables[n], total)
        if n:
            total = ring(total)

    mixer_out = mixer(mixer_input, mixer_gain, group_weight, mixer_scale)
    return (mixer_out, total)


def solution(mesh):
    placed = (
        P(("ep", "tp"), None),
        P(),
        P(),
        P(),
        P(("ep", "tp"), None),
        P(),
        P(("ep", "tp"), None),
        P(("ep", "tp"), None),
        P("ep", None, "tp"),
        P("ep", None, "tp"),
        P("ep", "tp", None),
    )

    return jax.shard_map(
        on_device,
        mesh=mesh,
        in_specs=placed,
        out_specs=(P(("ep", "tp"), None), P(("ep", "tp"), None)),
        check_vma=False,
    )
```

```python
import jax
import jax.numpy as jnp
from jax import lax
from jax.experimental import pallas as pl
from jax.experimental.pallas import tpu as pltpu
from jax.sharding import PartitionSpec as P

epsilon = 1e-06


def padded_2(value, sides, width):
    for axis, dim in sides:
        size, length = (lax.axis_size(axis), value.shape[dim])
        up = [(i, (i + 1) % size) for i in range(size - 1)]
        down = [(j, i) for i, j in up]
        last = lax.slice_in_dim(value, length - width, length, axis=dim)
        leading = lax.slice_in_dim(value, 0, width, axis=dim)
        before = lax.ppermute(last, axis, up)
        after = lax.ppermute(leading, axis, down)
        value = jnp.concatenate([before, value, after], axis=dim)
    return value


def normalize(row_values, gain):
    values = row_values.astype(jnp.float32)
    scaled = values * lax.rsqrt(jnp.mean(values * values, axis=-1, keepdims=True) + epsilon)
    return (scaled * gain).astype(jnp.bfloat16)


def pool_groups(padded, start_row, row_count, seq_length):
    group_width = padded.shape[1] // 4
    position = start_row + jnp.arange(row_count, dtype=jnp.int32)
    centre = padded[8 : 8 + row_count]
    pooled_parts = []
    for group_index in range(4):
        window = 2 ** (group_index + 1)
        reach_left = window // 2
        reach_right = window - 1 - reach_left
        group_cols = padded[:, group_index * group_width : (group_index + 1) * group_width]
        window_sum = group_cols[8 - reach_left : 8 - reach_left + row_count]
        for offset in range(1 - reach_left, reach_right + 1):
            window_sum = window_sum + group_cols[8 + offset : 8 + offset + row_count]
        cover = (
            jnp.minimum(position + reach_right + 1, seq_length)
            - jnp.maximum(position - reach_left, 0)
        ).astype(jnp.float32)
        pooled_parts.append(
            window_sum / cover[:, None]
            - centre[:, group_index * group_width : (group_index + 1) * group_width]
        )
    return jnp.stack(pooled_parts, axis=1).astype(jnp.bfloat16)


def mixer(mixer_input, mixer_gain, group_weight, mixer_scale):
    row_count = mixer_input.shape[0]
    normed = normalize(mixer_input, mixer_gain)
    padded = padded_2(normed, ((("ep", "tp"), 0),), 8)
    start_row = lax.axis_index(("ep", "tp")) * row_count
    seq_length = row_count * lax.axis_size(("ep", "tp"))
    pooled = pool_groups(padded.astype(jnp.float32), start_row, row_count, seq_length)
    mixed_groups = jnp.einsum(
        "tgi,gio->tgo", pooled, group_weight, preferred_element_type=jnp.float32
    )
    return (mixed_groups.reshape(row_count, -1) * mixer_scale).astype(jnp.bfloat16)


CORES = 2


def ring(value, steps=1):
    size = lax.axis_size("tp")
    return lax.ppermute(value, "tp", [(i, (i + steps * CORES) % size) for i in range(size)])


def core_swap(value):
    size = lax.axis_size("tp")
    return lax.ppermute(value, "tp", [(i, i ^ 1) for i in range(size)])


def is_direct(experts):
    return experts <= 4


def exchange(pieces):
    count = len(pieces)
    if is_direct(count):
        received = {
            m: lax.ppermute(pieces[m], "ep", [(i, i ^ m) for i in range(count)])
            for m in reversed(range(1, count))
        }
        return [pieces[0]] + [received[m] for m in range(1, count)]
    joined = lax.all_to_all(
        jnp.stack(pieces), "ep", split_axis=0, concat_axis=0, tiled=True
    )
    return [joined[m] for m in range(count)]


def route_table(routes, route_weight, experts, capacity):
    row_count, top_count = routes.shape
    named = routes.T
    if is_direct(experts):
        named = named ^ lax.axis_index("ep")
    member = jnp.zeros((experts, row_count), jnp.float32)
    expert_ids = jnp.arange(experts, dtype=jnp.int32)[:, None]
    for k in range(top_count):
        member = member + (named[k][None, :] == expert_ids)
    earlier = (
        jnp.arange(row_count, dtype=jnp.int32)[:, None]
        < jnp.arange(row_count, dtype=jnp.int32)[None, :]
    )
    place = jnp.dot(
        member.astype(jnp.bfloat16),
        earlier.astype(jnp.bfloat16),
        preferred_element_type=jnp.float32,
    )
    place = place + expert_ids.astype(jnp.float32) * capacity
    slots = [
        jnp.sum(jnp.where(named[k][None, :] == expert_ids, place, 0.0), axis=0)
        for k in range(top_count)
    ]
    return jnp.concatenate([jnp.stack(slots), route_weight.T], axis=0)


def slot_hits(table_ref, top_count, first, capacity):
    row_count = table_ref.shape[1]
    ids = lax.broadcasted_iota(jnp.int32, (capacity, row_count), 0) + first
    ids = ids.astype(jnp.float32)
    return [table_ref[k : k + 1, :] == ids for k in range(top_count)]


def dispatch(rows, table, experts, capacity):
    top_count = table.shape[0] // 2

    def kernel(rows_ref, table_ref, *out_refs):
        for m, out_ref in enumerate(out_refs):
            hits = slot_hits(table_ref, top_count, m * capacity, capacity)
            chosen = jnp.zeros(hits[0].shape, jnp.float32)
            for hit in hits:
                chosen = chosen + jnp.where(hit, 1.0, 0.0)
            out_ref[...] = jnp.dot(
                chosen.astype(jnp.bfloat16),
                rows_ref[...],
                preferred_element_type=jnp.float32,
            ).astype(jnp.bfloat16)

    shape = jax.ShapeDtypeStruct((capacity, rows.shape[1]), jnp.bfloat16)
    work = experts * capacity * rows.shape[0] * rows.shape[1]
    return pl.pallas_call(
        kernel,
        out_shape=[shape] * experts,
        cost_estimate=pl.CostEstimate(
            flops=2 * work, transcendentals=0, bytes_accessed=2 * rows.size + 2 * experts * shape.size
        ),
        name="dispatch",
    )(rows, table)


def combine(pieces, table):
    top_count = table.shape[0] // 2
    capacity, width = pieces[0].shape
    row_count = table.shape[1]

    def kernel(table_ref, *refs):
        out_ref = refs[-1]
        total = jnp.zeros((row_count, width), jnp.float32)
        for m in range(len(pieces)):
            hits = slot_hits(table_ref, top_count, m * capacity, capacity)
            weight = jnp.zeros(hits[0].shape, jnp.float32)
            for k, hit in enumerate(hits):
                weight = weight + jnp.where(hit, table_ref[top_count + k : top_count + k + 1, :], 0.0)
            high = weight.astype(jnp.bfloat16)
            low = (weight - high.astype(jnp.float32)).astype(jnp.bfloat16)
            for part in (high, low):
                total = total + lax.dot_general(
                    part,
                    refs[m][...],
                    (((0,), (0,)), ((), ())),
                    preferred_element_type=jnp.float32,
                )
        out_ref[...] = total

    work = len(pieces) * capacity * row_count * width
    return pl.pallas_call(
        kernel,
        out_shape=jax.ShapeDtypeStruct((row_count, width), jnp.float32),
        cost_estimate=pl.CostEstimate(
            flops=4 * work, transcendentals=0, bytes_accessed=2 * (len(pieces) * capacity + 2 * row_count) * width
        ),
        name="combine",
    )(table, *pieces)


def ffn(pieces, shards):
    count = len(pieces)
    capacity, width = pieces[0].shape
    rows = count * capacity
    hidden_width = shards[0][0].shape[1]
    tile = min(256, hidden_width)
    steps = hidden_width // tile
    n_shards = len(shards)

    def kernel(*refs):
        piece_refs = refs[:count]
        weight_refs = refs[count : count + 3 * n_shards]
        out_refs = refs[count + 3 * n_shards : 2 * count + 3 * n_shards]
        rows_ref, sum_ref = refs[-2:]
        step = pl.program_id(0)

        @pl.when(step == 0)
        def _():
            for m in range(count):
                rows_ref[m * capacity : (m + 1) * capacity, :] = piece_refs[m][...]

        values = rows_ref[...]
        term = None
        for n in range(n_shards):
            gate_ref, up_ref, down_ref = weight_refs[3 * n : 3 * n + 3]
            gate = jnp.dot(values, gate_ref[...], preferred_element_type=jnp.float32)
            up = jnp.dot(values, up_ref[...], preferred_element_type=jnp.float32)
            half_gate = 0.5 * gate
            silu = half_gate + half_gate * jnp.tanh(half_gate)
            hidden = (silu * up).astype(jnp.bfloat16)
            part = jnp.dot(hidden, down_ref[...], preferred_element_type=jnp.float32)
            term = part if term is None else term + part

        @pl.when(step == 0)
        def _():
            sum_ref[...] = term

        @pl.when(step > 0)
        def _():
            sum_ref[...] += term

        @pl.when(step == steps - 1)
        def _():
            for m in range(count):
                out_refs[m][...] = sum_ref[m * capacity : (m + 1) * capacity, :].astype(jnp.bfloat16)

    whole = pl.BlockSpec((capacity, width), lambda j: (0, 0))
    across = pl.BlockSpec((width, tile), lambda j: (0, j))
    along = pl.BlockSpec((tile, width), lambda j: (j, 0))
    work = rows * width * hidden_width * n_shards
    return pl.pallas_call(
        kernel,
        grid=(steps,),
        in_specs=[whole] * count + [across, across, along] * n_shards,
        out_specs=[whole] * count,
        out_shape=[jax.ShapeDtypeStruct((capacity, width), jnp.bfloat16)] * count,
        scratch_shapes=[
            pltpu.VMEM((rows, width), jnp.bfloat16),
            pltpu.VMEM((rows, width), jnp.float32),
        ],
        cost_estimate=pl.CostEstimate(
            flops=6 * work, transcendentals=rows * hidden_width * n_shards,
            bytes_accessed=4 * rows * width + 6 * width * hidden_width * n_shards,
        ),
        name="ffn",
    )(*pieces, *(w for shard in shards for w in shard))


def on_device(
    mixer_input,
    mixer_gain,
    group_weight,
    mixer_scale,
    expert_input,
    expert_gain,
    routes,
    route_weight,
    w_gate,
    w_up,
    w_down,
):
    row_count, top_count = routes.shape
    experts = lax.axis_size("ep") * w_gate.shape[0]
    capacity = 3 * top_count * row_count // (2 * experts)
    capacity = -(-capacity // 16) * 16
    chips = lax.axis_size("tp") // CORES

    normed = normalize(expert_input, expert_gain)
    shard = (w_gate[0], w_up[0], w_down[0])
    shards = [shard, tuple(core_swap(w) for w in shard)]

    table = route_table(routes, route_weight, experts, capacity)
    blocks = [normed]
    for _ in range(1, chips):
        blocks.append(ring(blocks[-1]))
    tables = [table] + [ring(table, n) for n in range(1, chips)]

    arrived = []
    for n in range(chips):
        arrived.append(exchange(dispatch(blocks[n], tables[n], experts, capacity)))

    order = list(range(1, chips)) + [0]
    back = {}
    for first in range(0, chips, 2):
        group = order[first : first + 2]
        served = ffn([piece for n in group for piece in arrived[n]], shards)
        for place, n in enumerate(group):
            back[n] = exchange(served[place * experts : (place + 1) * experts])

    total = None
    for n in order:
        term = combine(back[n], tables[n])
        total = term if total is None else term + total.astype(jnp.float32)
        total = total.astype(jnp.bfloat16)
        if n:
            total = ring(total)

    mixer_out = mixer(mixer_input, mixer_gain, group_weight, mixer_scale)
    return (mixer_out, total)


def solution(mesh):
    placed = (
        P(("ep", "tp"), None),
        P(),
        P(),
        P(),
        P(("ep", "tp"), None),
        P(),
        P(("ep", "tp"), None),
        P(("ep", "tp"), None),
        P("ep", None, "tp"),
        P("ep", None, "tp"),
        P("ep", "tp", None),
    )


    return jax.shard_map(
        on_device,
        mesh=mesh,
        in_specs=placed,
        out_specs=(P(("ep", "tp"), None), P(("ep", "tp"), None)),
        check_vma=False,
    )
```

```python
import jax
import jax.numpy as jnp
from jax import lax
from jax.experimental import pallas as pl
from jax.experimental.pallas import tpu as pltpu
from jax.sharding import PartitionSpec as P

epsilon = 1e-06


def padded_2(value, sides, width):
    for axis, dim in sides:
        size, length = (lax.axis_size(axis), value.shape[dim])
        up = [(i, (i + 1) % size) for i in range(size - 1)]
        down = [(j, i) for i, j in up]
        last = lax.slice_in_dim(value, length - width, length, axis=dim)
        leading = lax.slice_in_dim(value, 0, width, axis=dim)
        before = lax.ppermute(last, axis, up)
        after = lax.ppermute(leading, axis, down)
        value = jnp.concatenate([before, value, after], axis=dim)
    return value


def normalize(row_values, gain):
    values = row_values.astype(jnp.float32)
    scaled = values * lax.rsqrt(jnp.mean(values * values, axis=-1, keepdims=True) + epsilon)
    return (scaled * gain).astype(jnp.bfloat16)


def pool_groups(padded, start_row, row_count, seq_length):
    group_width = padded.shape[1] // 4
    position = start_row + jnp.arange(row_count, dtype=jnp.int32)
    centre = padded[8 : 8 + row_count]
    pooled_parts = []
    for group_index in range(4):
        window = 2 ** (group_index + 1)
        reach_left = window // 2
        reach_right = window - 1 - reach_left
        group_cols = padded[:, group_index * group_width : (group_index + 1) * group_width]
        window_sum = group_cols[8 - reach_left : 8 - reach_left + row_count]
        for offset in range(1 - reach_left, reach_right + 1):
            window_sum = window_sum + group_cols[8 + offset : 8 + offset + row_count]
        cover = (
            jnp.minimum(position + reach_right + 1, seq_length)
            - jnp.maximum(position - reach_left, 0)
        ).astype(jnp.float32)
        pooled_parts.append(
            window_sum / cover[:, None]
            - centre[:, group_index * group_width : (group_index + 1) * group_width]
        )
    return jnp.stack(pooled_parts, axis=1).astype(jnp.bfloat16)


def mixer(mixer_input, mixer_gain, group_weight, mixer_scale):
    row_count = mixer_input.shape[0]
    normed = normalize(mixer_input, mixer_gain)
    padded = padded_2(normed, ((("ep", "tp"), 0),), 8)
    start_row = lax.axis_index(("ep", "tp")) * row_count
    seq_length = row_count * lax.axis_size(("ep", "tp"))
    pooled = pool_groups(padded.astype(jnp.float32), start_row, row_count, seq_length)
    mixed_groups = jnp.einsum(
        "tgi,gio->tgo", pooled, group_weight, preferred_element_type=jnp.float32
    )
    return (mixed_groups.reshape(row_count, -1) * mixer_scale).astype(jnp.bfloat16)


CORES = 2


def shift(value, steps):
    size = lax.axis_size("tp")
    return lax.ppermute(value, "tp", [(i, (i + steps * CORES) % size) for i in range(size)])


def serving_order(chips):
    relayed = [n for even in range(2, chips, 2) for n in (even, even - 1)]
    return relayed + [n for n in range(1, chips) if n not in relayed] + [0]


def core_swap(value):
    size = lax.axis_size("tp")
    return lax.ppermute(value, "tp", [(i, i ^ 1) for i in range(size)])


def is_direct(experts):
    return experts <= 4


def exchange(pieces):
    count = len(pieces)
    if is_direct(count):
        received = {
            m: lax.ppermute(pieces[m], "ep", [(i, i ^ m) for i in range(count)])
            for m in reversed(range(1, count))
        }
        return [pieces[0]] + [received[m] for m in range(1, count)]
    joined = lax.all_to_all(
        jnp.stack(pieces), "ep", split_axis=0, concat_axis=0, tiled=True
    )
    return [joined[m] for m in range(count)]


def route_table(routes, route_weight, experts, capacity):
    row_count, top_count = routes.shape
    named = routes.T
    if is_direct(experts):
        named = named ^ lax.axis_index("ep")
    member = jnp.zeros((experts, row_count), jnp.float32)
    expert_ids = jnp.arange(experts, dtype=jnp.int32)[:, None]
    for k in range(top_count):
        member = member + (named[k][None, :] == expert_ids)
    earlier = (
        jnp.arange(row_count, dtype=jnp.int32)[:, None]
        < jnp.arange(row_count, dtype=jnp.int32)[None, :]
    )
    place = jnp.dot(
        member.astype(jnp.bfloat16),
        earlier.astype(jnp.bfloat16),
        preferred_element_type=jnp.float32,
    )
    place = place + expert_ids.astype(jnp.float32) * capacity
    slots = [
        jnp.sum(jnp.where(named[k][None, :] == expert_ids, place, 0.0), axis=0)
        for k in range(top_count)
    ]
    return jnp.concatenate([jnp.stack(slots), route_weight.T], axis=0)


def slot_hits(table_ref, top_count, first, capacity):
    row_count = table_ref.shape[1]
    ids = lax.broadcasted_iota(jnp.int32, (capacity, row_count), 0) + first
    ids = ids.astype(jnp.float32)
    return [table_ref[k : k + 1, :] == ids for k in range(top_count)]


def dispatch(rows, table, experts, capacity):
    top_count = table.shape[0] // 2

    def kernel(rows_ref, table_ref, *out_refs):
        for m, out_ref in enumerate(out_refs):
            hits = slot_hits(table_ref, top_count, m * capacity, capacity)
            chosen = jnp.zeros(hits[0].shape, jnp.float32)
            for hit in hits:
                chosen = chosen + jnp.where(hit, 1.0, 0.0)
            out_ref[...] = jnp.dot(
                chosen.astype(jnp.bfloat16),
                rows_ref[...],
                preferred_element_type=jnp.float32,
            ).astype(jnp.bfloat16)

    shape = jax.ShapeDtypeStruct((capacity, rows.shape[1]), jnp.bfloat16)
    work = experts * capacity * rows.shape[0] * rows.shape[1]
    return pl.pallas_call(
        kernel,
        out_shape=[shape] * experts,
        cost_estimate=pl.CostEstimate(
            flops=2 * work, transcendentals=0, bytes_accessed=2 * rows.size + 2 * experts * shape.size
        ),
        name="dispatch",
    )(rows, table)


def combine(pieces, table, others=()):
    top_count = table.shape[0] // 2
    capacity, width = pieces[0].shape
    row_count = table.shape[1]

    def kernel(table_ref, *refs):
        out_ref = refs[-1]
        total = jnp.zeros((row_count, width), jnp.float32)
        for other_ref in refs[len(pieces) : -1]:
            total = total + other_ref[...].astype(jnp.float32)
        for m in range(len(pieces)):
            hits = slot_hits(table_ref, top_count, m * capacity, capacity)
            weight = jnp.zeros(hits[0].shape, jnp.float32)
            for k, hit in enumerate(hits):
                weight = weight + jnp.where(hit, table_ref[top_count + k : top_count + k + 1, :], 0.0)
            high = weight.astype(jnp.bfloat16)
            low = (weight - high.astype(jnp.float32)).astype(jnp.bfloat16)
            for part in (high, low):
                total = total + lax.dot_general(
                    part,
                    refs[m][...],
                    (((0,), (0,)), ((), ())),
                    preferred_element_type=jnp.float32,
                )
        out_ref[...] = total.astype(jnp.bfloat16)

    work = len(pieces) * capacity * row_count * width
    return pl.pallas_call(
        kernel,
        out_shape=jax.ShapeDtypeStruct((row_count, width), jnp.bfloat16),
        cost_estimate=pl.CostEstimate(
            flops=4 * work, transcendentals=0, bytes_accessed=2 * (len(pieces) * capacity + 2 * row_count) * width
        ),
        name="combine",
    )(table, *pieces, *others)


def ffn(pieces, shards):
    count = len(pieces)
    capacity, width = pieces[0].shape
    rows = count * capacity
    hidden_width = shards[0][0].shape[1]
    tile = min(256, hidden_width)
    steps = hidden_width // tile
    n_shards = len(shards)

    def kernel(*refs):
        piece_refs = refs[:count]
        weight_refs = refs[count : count + 3 * n_shards]
        out_refs = refs[count + 3 * n_shards : 2 * count + 3 * n_shards]
        rows_ref, sum_ref = refs[-2:]
        step = pl.program_id(0)

        @pl.when(step == 0)
        def _():
            for m in range(count):
                rows_ref[m * capacity : (m + 1) * capacity, :] = piece_refs[m][...]

        values = rows_ref[...]
        term = None
        for n in range(n_shards):
            gate_ref, up_ref, down_ref = weight_refs[3 * n : 3 * n + 3]
            gate = jnp.dot(values, gate_ref[...], preferred_element_type=jnp.float32)
            up = jnp.dot(values, up_ref[...], preferred_element_type=jnp.float32)
            half_gate = 0.5 * gate
            silu = half_gate + half_gate * jnp.tanh(half_gate)
            hidden = (silu * up).astype(jnp.bfloat16)
            part = jnp.dot(hidden, down_ref[...], preferred_element_type=jnp.float32)
            term = part if term is None else term + part

        @pl.when(step == 0)
        def _():
            sum_ref[...] = term

        @pl.when(step > 0)
        def _():
            sum_ref[...] += term

        @pl.when(step == steps - 1)
        def _():
            for m in range(count):
                out_refs[m][...] = sum_ref[m * capacity : (m + 1) * capacity, :].astype(jnp.bfloat16)

    whole = pl.BlockSpec((capacity, width), lambda j: (0, 0))
    across = pl.BlockSpec((width, tile), lambda j: (0, j))
    along = pl.BlockSpec((tile, width), lambda j: (j, 0))
    work = rows * width * hidden_width * n_shards
    return pl.pallas_call(
        kernel,
        grid=(steps,),
        in_specs=[whole] * count + [across, across, along] * n_shards,
        out_specs=[whole] * count,
        out_shape=[jax.ShapeDtypeStruct((capacity, width), jnp.bfloat16)] * count,
        scratch_shapes=[
            pltpu.VMEM((rows, width), jnp.bfloat16),
            pltpu.VMEM((rows, width), jnp.float32),
        ],
        cost_estimate=pl.CostEstimate(
            flops=6 * work, transcendentals=rows * hidden_width * n_shards,
            bytes_accessed=4 * rows * width + 6 * width * hidden_width * n_shards,
        ),
        name="ffn",
    )(*pieces, *(w for shard in shards for w in shard))


def on_device(
    mixer_input,
    mixer_gain,
    group_weight,
    mixer_scale,
    expert_input,
    expert_gain,
    routes,
    route_weight,
    w_gate,
    w_up,
    w_down,
):
    row_count, top_count = routes.shape
    experts = lax.axis_size("ep") * w_gate.shape[0]
    capacity = 3 * top_count * row_count // (2 * experts)
    capacity = -(-capacity // 16) * 16
    chips = lax.axis_size("tp") // CORES

    normed = normalize(expert_input, expert_gain)
    shard = (w_gate[0], w_up[0], w_down[0])
    shards = [shard, tuple(core_swap(w) for w in shard)]

    order = serving_order(chips)
    table = route_table(routes, route_weight, experts, capacity)
    blocks, tables = {0: normed}, {0: table}
    for n in range(1, chips):
        blocks[n] = shift(normed, n) if n % 2 else shift(blocks[n - 1], 1)
        tables[n] = shift(table, n)

    arrived = {}
    for n in range(chips):
        arrived[n] = exchange(dispatch(blocks[n], tables[n], experts, capacity))

    back = {}
    for first in range(0, chips, 2):
        group = order[first : first + 2]
        served = ffn([piece for n in group for piece in arrived[n]], shards)
        for place, n in enumerate(group):
            back[n] = exchange(served[place * experts : (place + 1) * experts])

    home, relayed = [], {}
    for n in order[:-1]:
        term = combine(back[n], tables[n], relayed.get(n, ()))
        if n % 2:
            home.append(shift(term, -n))
        else:
            relayed[n - 1] = (shift(term, -1),)
    expert_out = combine(back[0], tables[0], home)

    mixer_out = mixer(mixer_input, mixer_gain, group_weight, mixer_scale)
    return (mixer_out, expert_out)


def solution(mesh):
    placed = (
        P(("ep", "tp"), None),
        P(),
        P(),
        P(),
        P(("ep", "tp"), None),
        P(),
        P(("ep", "tp"), None),
        P(("ep", "tp"), None),
        P("ep", None, "tp"),
        P("ep", None, "tp"),
        P("ep", "tp", None),
    )


    return jax.shard_map(
        on_device,
        mesh=mesh,
        in_specs=placed,
        out_specs=(P(("ep", "tp"), None), P(("ep", "tp"), None)),
        check_vma=False,
    )
```

```python
import jax
import jax.numpy as jnp
from jax import lax
from jax.experimental import pallas as pl
from jax.experimental.pallas import tpu as pltpu
from jax.sharding import PartitionSpec as P

epsilon = 1e-06


def padded_2(value, sides, width):
    for axis, dim in sides:
        size, length = (lax.axis_size(axis), value.shape[dim])
        up = [(i, (i + 1) % size) for i in range(size - 1)]
        down = [(j, i) for i, j in up]
        last = lax.slice_in_dim(value, length - width, length, axis=dim)
        leading = lax.slice_in_dim(value, 0, width, axis=dim)
        before = lax.ppermute(last, axis, up)
        after = lax.ppermute(leading, axis, down)
        value = jnp.concatenate([before, value, after], axis=dim)
    return value


def normalize(row_values, gain):
    values = row_values.astype(jnp.float32)
    scaled = values * lax.rsqrt(jnp.mean(values * values, axis=-1, keepdims=True) + epsilon)
    return (scaled * gain).astype(jnp.bfloat16)


def pool_groups(padded, start_row, row_count, seq_length):
    group_width = padded.shape[1] // 4
    position = start_row + jnp.arange(row_count, dtype=jnp.int32)
    centre = padded[8 : 8 + row_count]
    pooled_parts = []
    for group_index in range(4):
        window = 2 ** (group_index + 1)
        reach_left = window // 2
        reach_right = window - 1 - reach_left
        group_cols = padded[:, group_index * group_width : (group_index + 1) * group_width]
        window_sum = group_cols[8 - reach_left : 8 - reach_left + row_count]
        for offset in range(1 - reach_left, reach_right + 1):
            window_sum = window_sum + group_cols[8 + offset : 8 + offset + row_count]
        cover = (
            jnp.minimum(position + reach_right + 1, seq_length)
            - jnp.maximum(position - reach_left, 0)
        ).astype(jnp.float32)
        pooled_parts.append(
            window_sum / cover[:, None]
            - centre[:, group_index * group_width : (group_index + 1) * group_width]
        )
    return jnp.stack(pooled_parts, axis=1).astype(jnp.bfloat16)


def mixer(mixer_input, mixer_gain, group_weight, mixer_scale):
    row_count = mixer_input.shape[0]
    normed = normalize(mixer_input, mixer_gain)
    padded = padded_2(normed, ((("ep", "tp"), 0),), 8)
    start_row = lax.axis_index(("ep", "tp")) * row_count
    seq_length = row_count * lax.axis_size(("ep", "tp"))
    pooled = pool_groups(padded.astype(jnp.float32), start_row, row_count, seq_length)
    mixed_groups = jnp.einsum(
        "tgi,gio->tgo", pooled, group_weight, preferred_element_type=jnp.float32
    )
    return (mixed_groups.reshape(row_count, -1) * mixer_scale).astype(jnp.bfloat16)


CORES = 2


def shift(value, steps):
    size = lax.axis_size("tp")
    return lax.ppermute(value, "tp", [(i, (i + steps * CORES) % size) for i in range(size)])


def serving_order(chips):
    relayed = [n for even in range(2, chips, 2) for n in (even, even - 1)]
    return relayed + [n for n in range(1, chips) if n not in relayed] + [0]


def serving_groups(order):
    pairs = [order[n : n + 2] for n in range(2, len(order), 2)]
    return [[order[1]], [order[0]]] + pairs


def core_swap(value):
    size = lax.axis_size("tp")
    return lax.ppermute(value, "tp", [(i, i ^ 1) for i in range(size)])


def is_direct(experts):
    return experts <= 4


def exchange(pieces):
    count = len(pieces)
    if is_direct(count):
        received = {
            m: lax.ppermute(pieces[m], "ep", [(i, i ^ m) for i in range(count)])
            for m in reversed(range(1, count))
        }
        return [pieces[0]] + [received[m] for m in range(1, count)]
    joined = lax.all_to_all(
        jnp.stack(pieces), "ep", split_axis=0, concat_axis=0, tiled=True
    )
    return [joined[m] for m in range(count)]


def route_table(routes, route_weight, experts, capacity):
    row_count, top_count = routes.shape
    named = routes.T
    if is_direct(experts):
        named = named ^ lax.axis_index("ep")
    member = jnp.zeros((experts, row_count), jnp.float32)
    expert_ids = jnp.arange(experts, dtype=jnp.int32)[:, None]
    for k in range(top_count):
        member = member + (named[k][None, :] == expert_ids)
    earlier = (
        jnp.arange(row_count, dtype=jnp.int32)[:, None]
        < jnp.arange(row_count, dtype=jnp.int32)[None, :]
    )
    place = jnp.dot(
        member.astype(jnp.bfloat16),
        earlier.astype(jnp.bfloat16),
        preferred_element_type=jnp.float32,
    )
    place = place + expert_ids.astype(jnp.float32) * capacity
    slots = [
        jnp.sum(jnp.where(named[k][None, :] == expert_ids, place, 0.0), axis=0)
        for k in range(top_count)
    ]
    return jnp.concatenate([jnp.stack(slots), route_weight.T], axis=0)


def slot_hits(table_ref, top_count, first, capacity):
    row_count = table_ref.shape[1]
    ids = lax.broadcasted_iota(jnp.int32, (capacity, row_count), 0) + first
    ids = ids.astype(jnp.float32)
    return [table_ref[k : k + 1, :] == ids for k in range(top_count)]


def dispatch(rows, table, experts, capacity):
    top_count = table.shape[0] // 2

    def kernel(rows_ref, table_ref, *out_refs):
        for m, out_ref in enumerate(out_refs):
            hits = slot_hits(table_ref, top_count, m * capacity, capacity)
            chosen = jnp.zeros(hits[0].shape, jnp.float32)
            for hit in hits:
                chosen = chosen + jnp.where(hit, 1.0, 0.0)
            out_ref[...] = jnp.dot(
                chosen.astype(jnp.bfloat16),
                rows_ref[...],
                preferred_element_type=jnp.float32,
            ).astype(jnp.bfloat16)

    shape = jax.ShapeDtypeStruct((capacity, rows.shape[1]), jnp.bfloat16)
    work = experts * capacity * rows.shape[0] * rows.shape[1]
    return pl.pallas_call(
        kernel,
        out_shape=[shape] * experts,
        cost_estimate=pl.CostEstimate(
            flops=2 * work, transcendentals=0, bytes_accessed=2 * rows.size + 2 * experts * shape.size
        ),
        name="dispatch",
    )(rows, table)


def combine(pieces, table, others, kind):
    top_count = table.shape[0] // 2
    capacity, width = pieces[0].shape
    row_count = table.shape[1]

    def kernel(table_ref, *refs):
        out_ref = refs[-1]
        total = jnp.zeros((row_count, width), jnp.float32)
        for other_ref in refs[len(pieces) : -1]:
            total = total + other_ref[...].astype(jnp.float32)
        for m in range(len(pieces)):
            hits = slot_hits(table_ref, top_count, m * capacity, capacity)
            weight = jnp.zeros(hits[0].shape, jnp.float32)
            for k, hit in enumerate(hits):
                weight = weight + jnp.where(hit, table_ref[top_count + k : top_count + k + 1, :], 0.0)
            high = weight.astype(jnp.bfloat16)
            low = (weight - high.astype(jnp.float32)).astype(jnp.bfloat16)
            for part in (high, low):
                total = total + lax.dot_general(
                    part,
                    refs[m][...],
                    (((0,), (0,)), ((), ())),
                    preferred_element_type=jnp.float32,
                )
        out_ref[...] = total.astype(kind)

    work = len(pieces) * capacity * row_count * width
    return pl.pallas_call(
        kernel,
        out_shape=jax.ShapeDtypeStruct((row_count, width), kind),
        cost_estimate=pl.CostEstimate(
            flops=4 * work, transcendentals=0, bytes_accessed=2 * (len(pieces) * capacity + 2 * row_count) * width
        ),
        name="combine",
    )(table, *pieces, *others)


def ffn(pieces, shards):
    count = len(pieces)
    capacity, width = pieces[0].shape
    rows = count * capacity
    hidden_width = shards[0][0].shape[1]
    tile = min(256, hidden_width)
    steps = hidden_width // tile
    n_shards = len(shards)

    def kernel(*refs):
        piece_refs = refs[:count]
        weight_refs = refs[count : count + 3 * n_shards]
        out_refs = refs[count + 3 * n_shards : 2 * count + 3 * n_shards]
        rows_ref, sum_ref = refs[-2:]
        step = pl.program_id(0)

        @pl.when(step == 0)
        def _():
            for m in range(count):
                rows_ref[m * capacity : (m + 1) * capacity, :] = piece_refs[m][...]

        values = rows_ref[...]
        term = None
        for n in range(n_shards):
            gate_ref, up_ref, down_ref = weight_refs[3 * n : 3 * n + 3]
            gate = jnp.dot(values, gate_ref[...], preferred_element_type=jnp.float32)
            up = jnp.dot(values, up_ref[...], preferred_element_type=jnp.float32)
            half_gate = 0.5 * gate
            silu = half_gate + half_gate * jnp.tanh(half_gate)
            hidden = (silu * up).astype(jnp.bfloat16)
            part = jnp.dot(hidden, down_ref[...], preferred_element_type=jnp.float32)
            term = part if term is None else term + part

        @pl.when(step == 0)
        def _():
            sum_ref[...] = term

        @pl.when(step > 0)
        def _():
            sum_ref[...] += term

        @pl.when(step == steps - 1)
        def _():
            for m in range(count):
                out_refs[m][...] = sum_ref[m * capacity : (m + 1) * capacity, :].astype(jnp.bfloat16)

    whole = pl.BlockSpec((capacity, width), lambda j: (0, 0))
    across = pl.BlockSpec((width, tile), lambda j: (0, j))
    along = pl.BlockSpec((tile, width), lambda j: (j, 0))
    work = rows * width * hidden_width * n_shards
    return pl.pallas_call(
        kernel,
        grid=(steps,),
        in_specs=[whole] * count + [across, across, along] * n_shards,
        out_specs=[whole] * count,
        out_shape=[jax.ShapeDtypeStruct((capacity, width), jnp.bfloat16)] * count,
        scratch_shapes=[
            pltpu.VMEM((rows, width), jnp.bfloat16),
            pltpu.VMEM((rows, width), jnp.float32),
        ],
        cost_estimate=pl.CostEstimate(
            flops=6 * work, transcendentals=rows * hidden_width * n_shards,
            bytes_accessed=4 * rows * width + 6 * width * hidden_width * n_shards,
        ),
        name="ffn",
    )(*pieces, *(w for shard in shards for w in shard))


def on_device(
    mixer_input,
    mixer_gain,
    group_weight,
    mixer_scale,
    expert_input,
    expert_gain,
    routes,
    route_weight,
    w_gate,
    w_up,
    w_down,
):
    row_count, top_count = routes.shape
    experts = lax.axis_size("ep") * w_gate.shape[0]
    capacity = 3 * top_count * row_count // (2 * experts)
    capacity = -(-capacity // 16) * 16
    chips = lax.axis_size("tp") // CORES

    normed = normalize(expert_input, expert_gain)
    shard = (w_gate[0], w_up[0], w_down[0])
    shards = [shard, tuple(core_swap(w) for w in shard)]

    order = serving_order(chips)
    table = route_table(routes, route_weight, experts, capacity)
    blocks, tables = {0: normed}, {0: table}
    for n in range(1, chips):
        blocks[n] = shift(normed, n) if n % 2 else shift(blocks[n - 1], 1)
        tables[n] = shift(table, n)

    arrived = {}
    for n in range(chips):
        arrived[n] = exchange(dispatch(blocks[n], tables[n], experts, capacity))

    back = {}
    for group in serving_groups(order):
        served = ffn([piece for n in group for piece in arrived[n]], shards)
        for place, n in enumerate(group):
            back[n] = exchange(served[place * experts : (place + 1) * experts])

    home, relayed = [], {}
    for n in order[:-1]:
        term = combine(back[n], tables[n], relayed.get(n, ()), jnp.bfloat16)
        if n % 2:
            home.append(shift(term, -n))
        else:
            relayed[n - 1] = (shift(term, -1),)
    total = combine(back[0], tables[0], (), jnp.float32)
    for term in home:
        total = total + term.astype(jnp.float32)
    expert_out = total.astype(jnp.bfloat16)

    mixer_out = mixer(mixer_input, mixer_gain, group_weight, mixer_scale)
    return (mixer_out, expert_out)


def solution(mesh):
    placed = (
        P(("ep", "tp"), None),
        P(),
        P(),
        P(),
        P(("ep", "tp"), None),
        P(),
        P(("ep", "tp"), None),
        P(("ep", "tp"), None),
        P("ep", None, "tp"),
        P("ep", None, "tp"),
        P("ep", "tp", None),
    )


    return jax.shard_map(
        on_device,
        mesh=mesh,
        in_specs=placed,
        out_specs=(P(("ep", "tp"), None), P(("ep", "tp"), None)),
        check_vma=False,
    )
```
